32 devices in a mesh: rep: 4 (over z), fs: 4 (over y, x), tp: 2 (over core).
Axes of the slice: x: 2, y: 2, z: 4, core: 2. Of those that a mesh axis runs over, the one named last changes fastest.
Arguments:
- hidden_in: bfloat16 [2048, 2048], P('rep'), may hold values from -6 to 6
- cotangent: bfloat16 [2048, 2048], P('rep'), may hold values from -3 to 3
- w_up: bfloat16 [2048, 8192], P('rep', ('fs', 'tp')), may hold values from -0.125 to 0.125
- w_down: bfloat16 [8192, 2048], P(('fs', 'tp'), 'rep'), may hold values from -0.0625 to 0.0625
Outputs:
- input_grad: bfloat16 [2048, 2048], P('rep')
- up_grad: float32 [2048, 8192], P('rep', ('fs', 'tp'))
- down_grad: float32 [8192, 2048], P(('fs', 'tp'), 'rep')
The draws below stay inside these ranges and needn't reach their ends.
All inputs are finite; a program needn't handle non-finite values.
Results may differ from the reference program's by a relative error of at most 0.017.
Values may be sent and summed in bfloat16 or wider, within the bound.
No kernel may reach another device: no remote copies, remote signals or barrier semaphores. Data moves between devices by JAX's collectives and lax.ppermute only.
A program may use at most 64 MiB of HBM per device.

```python
import jax
import jax.numpy as jnp
from jax import lax

D = 2048
FF = 8192
TOKENS = 2048
N_FS = 4
N_TP = 2


def strengthened(drawn, key, source, target, parts, factor):
    def block_of(dim):
        return (jnp.arange(drawn.shape[dim]) // (drawn.shape[dim] // parts)).reshape((-1,) + (1,) * (drawn.ndim - 1 - dim))

    near = jax.random.permutation(key, parts)[block_of(target)]
    other_side = (block_of(target) + parts // 2) % parts
    return jnp.where((block_of(source) == near) | (block_of(source) == other_side), factor * drawn, drawn)


def level_of(stream_key, dims, pieces, low, largest):
    level = 1.0
    for position, parts in pieces:
        steps = jax.random.uniform(jax.random.fold_in(jax.random.fold_in(stream_key, 6), position), (parts,), jnp.float32, low / len(pieces), largest / len(pieces))
        level = level * jnp.repeat(jnp.exp(steps), dims[position] // parts).reshape((-1,) + (1,) * (len(dims) - 1 - position))
    return level


def noise(key, extent, width, reach, pieces=(), dtype=jnp.bfloat16):
    drawn = width * jax.random.normal(key, extent, jnp.float32)
    if pieces:
        drawn = drawn * level_of(key, extent, pieces, -0.22, 0.18)
    return jnp.clip(drawn, -reach, reach).astype(dtype)


def heavy_noise(key, shape, width, bound, split, heavy, kind=jnp.bfloat16):
    values = width * jax.random.normal(key, shape, jnp.float32)
    if split:
        values = values * level_of(key, shape, split, -0.22, 0.18)
    return jnp.clip(strengthened(values, jax.random.fold_in(key, 3), *heavy), -bound, bound).astype(kind)


def setup_inputs(seed: int = 0) -> dict:
    splits = jax.random.split(jax.random.key(seed), 5)
    hidden_in = heavy_noise(splits[0], (TOKENS, D), 1.0, 6.0, ((0, 4),), (0, 1, 4, 2.0))
    cotangent = heavy_noise(splits[1], (TOKENS, D), 0.5, 3.0, ((0, 4),), (0, 1, 4, 2.0))
    w_up = noise(splits[2], (D, FF), D ** -0.5, 0.125, ((0, 4), (1, 8)))
    w_down = noise(splits[3], (FF, D), FF ** -0.5, 0.0625, ((0, 8), (1, 4)))
    return dict(hidden_in=hidden_in, cotangent=cotangent, w_up=w_up, w_down=w_down)


def contract_last(left, right):
    return lax.dot_general(left, right, (((1,), (1,)), ((), ())), preferred_element_type=jnp.float32)


def contract_first(left, right):
    return lax.dot_general(left, right, (((0,), (0,)), ((), ())), preferred_element_type=jnp.float32)


def reference(hidden_in, cotangent, w_up, w_down):
    blocks = N_FS * N_TP
    block_cols = FF // blocks
    up_blocks = jnp.transpose(w_up.reshape(D, blocks, block_cols), (1, 0, 2))
    down_blocks = w_down.reshape(blocks, block_cols, D)

    def one_block(summed, weights):
        up_part, down_part = weights
        preact = jnp.dot(hidden_in, up_part, preferred_element_type=jnp.float32)
        back_grad = contract_last(cotangent, down_part)
        active = jnp.maximum(preact, 0.0)
        hidden = (active * active).astype(jnp.bfloat16)
        slopes = (2.0 * active * back_grad).astype(jnp.bfloat16)
        part_sum = lax.optimization_barrier(contract_last(slopes, up_part).astype(jnp.bfloat16))
        summed = summed + part_sum.astype(jnp.float32)
        grad_upper = contract_first(hidden_in, slopes)
        grad_lower = contract_first(hidden, cotangent)
        return summed, (grad_upper, grad_lower)

    summed, (grads_upper, grads_lower) = lax.scan(
        one_block, jnp.zeros((TOKENS, D), jnp.float32), (up_blocks, down_blocks))
    input_grad = summed.astype(jnp.bfloat16)
    up_grad = jnp.transpose(grads_upper, (1, 0, 2)).reshape(D, FF)
    down_grad = grads_lower.reshape(FF, D)
    return (input_grad, up_grad, down_grad)
```

```python
import jax
import jax.numpy as jnp
from jax import lax
from jax.sharding import PartitionSpec as P

BF16 = jnp.bfloat16
F32 = jnp.float32
GATHER_BUDGET = 20 << 20


def contract_last(left, right):
    return lax.dot_general(
        left, right, (((1,), (1,)), ((), ())), preferred_element_type=F32
    )


def contract_first(left, right):
    return lax.dot_general(
        left, right, (((0,), (0,)), ((), ())), preferred_element_type=F32
    )


def swap(value, axis, offset):
    size = lax.axis_size(axis)
    return lax.ppermute(value, axis, [(i, i ^ offset) for i in range(size)])


def bits_of(size):
    return [1 << k for k in range(size.bit_length() - 1)]


def gathered_weights(hidden_in, cotangent, w_up, w_down):
    up_full = lax.all_gather(w_up, "rep", axis=0, tiled=True)
    back_grad = contract_last(cotangent, lax.all_gather(w_down, "rep", axis=1, tiled=True))
    preact = jnp.dot(hidden_in, up_full, preferred_element_type=F32)
    active = jnp.maximum(preact, 0.0)
    hidden = (active * active).astype(BF16)
    slopes = (2.0 * active * back_grad).astype(BF16)
    grad_upper = lax.psum_scatter(
        contract_first(hidden_in, slopes).astype(BF16), "rep", scatter_dimension=0, tiled=True
    ).astype(F32)
    lower_rows = lax.psum_scatter(
        contract_first(cotangent, hidden).astype(BF16), "rep", scatter_dimension=0, tiled=True
    ).astype(F32)
    partial_sum = contract_last(slopes, up_full).astype(BF16)
    input_grad = lax.psum(partial_sum, ("fs", "tp"))
    return input_grad, grad_upper, lower_rows.T


def gathered_tokens(hidden_in, cotangent, w_up, w_down):
    n_rep, n_fs, n_tp = (lax.axis_size(a) for a in ("rep", "fs", "tp"))
    rep, fs, tp = (lax.axis_index(a) for a in ("rep", "fs", "tp"))
    n_plane = n_fs * n_tp
    place = tp * n_fs + fs
    tokens, width = hidden_in.shape
    part = tokens // n_plane
    shard = w_up.shape[0]
    cols = w_up.shape[1] // n_rep
    fs_bits, tp_bits, rep_bits = bits_of(n_fs), bits_of(n_tp), bits_of(n_rep)

    def relative(value):
        return [
            lax.dynamic_slice_in_dim(value, (place ^ b) * part, part, 0) for b in range(n_plane)
        ]

    def over_rep(piece):
        pieces = {0: piece}
        for offset in reversed(rep_bits):
            for j, v in list(pieces.items()):
                pieces[j | offset] = swap(v, "rep", offset)
        return pieces

    def over_plane(piece, order):
        blocks = {0: piece}
        for offset in order:
            for b, v in list(blocks.items()):
                blocks[b | offset] = swap(v, "fs", offset)
        rows = jnp.concatenate([blocks[b] for b in range(n_fs)], 0)
        for offset in tp_bits:
            rows = jnp.concatenate([rows, swap(rows, "tp", offset)], 0)
        return rows

    def all_tokens(value, order):
        own = relative(value)
        pieces = over_rep(own[0])
        return [jnp.concatenate(own, 0)] + [
            over_plane(pieces[j], order) for j in range(1, n_rep)
        ]

    hidden_rows = all_tokens(hidden_in, fs_bits)
    cot_rows = all_tokens(cotangent, fs_bits[::-1])

    def up_block(j):
        return lax.dynamic_slice_in_dim(w_up, (rep ^ j) * cols, cols, 1)

    def down_block(j):
        return lax.dynamic_slice_in_dim(w_down, (rep ^ j) * cols, cols, 0)

    up = jnp.zeros((shard * n_rep, cols), BF16)
    down = jnp.zeros((cols, shard * n_rep), BF16)
    for j in range(n_rep):
        u, d = up_block(j), down_block(j)
        if j:
            u, d = swap(u, "rep", j), swap(d, "rep", j)
        up = lax.dynamic_update_slice_in_dim(up, u, (rep ^ j) * shard, 0)
        down = lax.dynamic_update_slice_in_dim(down, d, (rep ^ j) * shard, 1)

    hidden_all = jnp.concatenate(hidden_rows, 0)
    cot_all = jnp.concatenate(cot_rows, 0)
    preact = jnp.dot(hidden_all, up, preferred_element_type=F32)
    back_grad = jnp.dot(cot_all, down.T, preferred_element_type=F32)
    active = jnp.maximum(preact, 0.0)
    hidden = (active * active).astype(BF16)
    slopes = (2.0 * active * back_grad).astype(BF16)

    half = width // 2

    def over_places(partial):
        keep = partial
        for offset in reversed(tp_bits):
            rows = keep.shape[0] // 2
            keep = keep[:rows] + swap(keep[rows:].astype(BF16), "tp", offset).astype(F32)
        halves = []
        for columns, order in ((slice(None, half), fs_bits), (slice(half, None), fs_bits[::-1])):
            blocks = {b: keep[b * part : (b + 1) * part, columns] for b in range(n_fs)}
            for offset in order:
                sent = [b for b in blocks if b & offset]
                got = swap(jnp.concatenate([blocks[b].astype(BF16) for b in sent], 0), "fs", offset)
                for k, b in enumerate(sent):
                    blocks[b ^ offset] = blocks[b ^ offset] + got[k * part : (k + 1) * part].astype(F32)
                    del blocks[b]
            halves.append(blocks[0])
        return jnp.concatenate(halves, 1)

    summed = {}
    for j in reversed(range(n_rep)):
        partial = contract_last(slopes[j * tokens : (j + 1) * tokens], up)
        summed[j] = over_places(partial)
    for offset in rep_bits:
        for j in [j for j in summed if j & offset]:
            summed[j ^ offset] = summed[j ^ offset] + swap(summed.pop(j).astype(BF16), "rep", offset).astype(F32)
    final = summed[0].astype(BF16)
    sides = []
    for columns, order in ((slice(None, half), fs_bits), (slice(half, None), fs_bits[::-1])):
        blocks = {0: final[:, columns]}
        for offset in order:
            for b, v in list(blocks.items()):
                blocks[b | offset] = swap(v, "fs", offset)
        sides.append(jnp.concatenate([blocks[b] for b in range(n_fs)], 0))
    rows = jnp.concatenate(sides, 1)
    for offset in tp_bits:
        rows = jnp.concatenate([rows, swap(rows, "tp", offset)], 0)
    input_grad = jnp.zeros((tokens, width), BF16)
    for b in range(n_plane):
        input_grad = lax.dynamic_update_slice_in_dim(
            input_grad, rows[b * part : (b + 1) * part], (place ^ b) * part, 0
        )

    up_own = contract_first(hidden_all, slopes).astype(BF16)
    down_own = contract_first(hidden, cot_all).astype(BF16)
    up_grad = jnp.zeros((shard, cols * n_rep), F32)
    down_grad = jnp.zeros((cols * n_rep, shard), F32)
    for j in range(n_rep):
        u = lax.dynamic_slice_in_dim(up_own, (rep ^ j) * shard, shard, 0)
        d = lax.dynamic_slice_in_dim(down_own, (rep ^ j) * shard, shard, 1)
        if j:
            u, d = swap(u, "rep", j), swap(d, "rep", j)
        up_grad = lax.dynamic_update_slice_in_dim(up_grad, u.astype(F32), (rep ^ j) * cols, 1)
        down_grad = lax.dynamic_update_slice_in_dim(down_grad, d.astype(F32), (rep ^ j) * cols, 0)
    return input_grad, up_grad, down_grad


def on_device(hidden_in, cotangent, w_up, w_down):
    gathered = 2 * hidden_in.size * lax.axis_size("rep") * hidden_in.dtype.itemsize
    plan = gathered_tokens if gathered <= GATHER_BUDGET else gathered_weights
    return plan(hidden_in, cotangent, w_up, w_down)


def solution(mesh):
    return jax.shard_map(
        on_device,
        mesh=mesh,
        in_specs=(P("rep", None), P("rep", None), P("rep", ("fs", "tp")), P(("fs", "tp"), "rep")),
        out_specs=(P("rep", None), P("rep", ("fs", "tp")), P(("fs", "tp"), "rep")),
        check_vma=False,
    )
```

```python
import functools

import jax
import jax.numpy as jnp
from jax import lax
from jax.experimental import pallas as pl
from jax.experimental.pallas import tpu as pltpu
from jax.sharding import PartitionSpec as P

BF16 = jnp.bfloat16
F32 = jnp.float32
GATHER_BUDGET = 20 << 20


def contract_last(left, right):
    return lax.dot_general(
        left, right, (((1,), (1,)), ((), ())), preferred_element_type=F32
    )


def contract_first(left, right):
    return lax.dot_general(
        left, right, (((0,), (0,)), ((), ())), preferred_element_type=F32
    )


def swap(value, axis, offset):
    size = lax.axis_size(axis)
    return lax.ppermute(value, axis, [(i, i ^ offset) for i in range(size)])


def gathered_weights(hidden_in, cotangent, w_up, w_down):
    up_full = lax.all_gather(w_up, "rep", axis=0, tiled=True)
    back_grad = contract_last(cotangent, lax.all_gather(w_down, "rep", axis=1, tiled=True))
    preact = jnp.dot(hidden_in, up_full, preferred_element_type=F32)
    active = jnp.maximum(preact, 0.0)
    hidden = (active * active).astype(BF16)
    slopes = (2.0 * active * back_grad).astype(BF16)
    grad_upper = lax.psum_scatter(
        contract_first(hidden_in, slopes).astype(BF16), "rep", scatter_dimension=0, tiled=True
    ).astype(F32)
    lower_rows = lax.psum_scatter(
        contract_first(cotangent, hidden).astype(BF16), "rep", scatter_dimension=0, tiled=True
    ).astype(F32)
    partial_sum = contract_last(slopes, up_full).astype(BF16)
    input_grad = lax.psum(partial_sum, ("fs", "tp"))
    return input_grad, grad_upper, lower_rows.T


def finish(ref, sem):
    pltpu.make_async_copy(ref, ref, sem).wait()


def gather_kernel(mine, theirs, planes, *refs):
    ins = (dict(zip(mine, refs)), dict(zip(theirs, refs[len(mine) :])))
    outs = refs[len(mine) + len(theirs) :][:2]
    sems = refs[-1]
    fs, tp = lax.axis_index("fs"), lax.axis_index("tp")
    part = outs[0].shape[0] // (8 * len(planes))
    for which, name in enumerate(("hidden_in", "cotangent")):
        for core in range(2):
            for k, plane in enumerate(planes):
                for b in range(4):
                    if plane == "own":
                        at = pl.multiple_of(((tp ^ core) * 4 + (fs ^ b)) * part, part)
                        src = ins[0][name].at[pl.ds(at, part), :]
                    elif b < 3:
                        src = ins[core][plane + "oxy"[b]].at[which * part : (which + 1) * part, :]
                    else:
                        src = ins[core][plane + "fg"[which]]
                    to = pl.ds(((core * len(planes) + k) * 4 + b) * part, part)
                    pltpu.make_async_copy(src, outs[which].at[to, :], sems.at[which]).start()
    finish(outs[0], sems.at[0])
    finish(outs[1], sems.at[1])


def gather_rows(mine, theirs, planes):
    tokens, width = mine["hidden_in"].shape
    pieces = [p + k for p in planes if p != "own" for k in "oxyfg"]
    whole = ["hidden_in", "cotangent"]
    any_space = pl.BlockSpec(memory_space=pl.ANY)
    out = pltpu.VMEM((len(planes) * tokens, width), BF16)
    return pl.pallas_call(
        functools.partial(gather_kernel, whole + pieces, pieces, planes),
        out_shape=[out, out],
        in_specs=[any_space] * (2 + 2 * len(pieces)),
        out_specs=[any_space] * 2,
        scratch_shapes=[pltpu.SemaphoreType.DMA((2,))],
        cost_estimate=pl.CostEstimate(flops=4_000_000_000, bytes_accessed=4 * tokens * width * len(planes), transcendentals=0),
        compiler_params=pltpu.CompilerParams(vmem_limit_bytes=1 << 20),
    )(*[mine[k] for k in whole + pieces], *[theirs[k] for k in pieces])


def weights_kernel(w_up, w_down, *refs):
    ups, downs, (up, down, sems) = refs[:3], refs[3:6], refs[6:]
    rep = lax.axis_index("rep")
    shard, cols = w_up.shape[0], up.shape[1]
    for j in range(4):
        at = pl.multiple_of((rep ^ j) * shard, shard)
        mine = pl.multiple_of(rep * cols, cols)
        u = ups[j - 1] if j else w_up.at[:, pl.ds(mine, cols)]
        d = downs[j - 1] if j else w_down.at[pl.ds(mine, cols), :]
        pltpu.make_async_copy(u, up.at[pl.ds(at, shard), :], sems.at[0]).start()
        pltpu.make_async_copy(d, down.at[:, pl.ds(at, shard)], sems.at[1]).start()
    finish(up, sems.at[0])
    finish(down, sems.at[1])


def gather_weights(w_up, w_down, ups, downs):
    (shard, cols), width = ups[0].shape, w_down.shape[1] * 4
    any_space = pl.BlockSpec(memory_space=pl.ANY)
    return pl.pallas_call(
        weights_kernel,
        out_shape=[pltpu.VMEM((width, cols), BF16), pltpu.VMEM((cols, width), BF16)],
        in_specs=[any_space] * 8,
        out_specs=[any_space] * 2,
        scratch_shapes=[pltpu.SemaphoreType.DMA((2,))],
        cost_estimate=pl.CostEstimate(flops=1_000_000_000, bytes_accessed=4 * width * cols, transcendentals=0),
        compiler_params=pltpu.CompilerParams(vmem_limit_bytes=1 << 20),
        name="weights",
    )(w_up, w_down, *ups, *downs)


def gathered_tokens(hidden_in, cotangent, w_up, w_down):
    n_rep, n_fs = lax.axis_size("rep"), lax.axis_size("fs")
    rep, fs, tp = (lax.axis_index(a) for a in ("rep", "fs", "tp"))
    tokens, width = hidden_in.shape
    side = tokens // 2
    part = side // n_fs
    half = width // 2
    shard = w_up.shape[0]
    cols = w_up.shape[1] // n_rep

    def rows_at(value, core, block, count=part):
        return lax.dynamic_slice_in_dim(value, core * side + block * part, count, 0)

    piece = jnp.concatenate([rows_at(hidden_in, tp, fs), rows_at(cotangent, tp, fs)], 0)
    near = swap(piece, "rep", 1)
    far = swap(piece, "rep", 2)
    across = swap(far, "rep", 1)

    ups, downs = [], []
    for j in range(1, n_rep):
        u = lax.dynamic_slice_in_dim(w_up, (rep ^ j) * cols, cols, 1)
        d = lax.dynamic_slice_in_dim(w_down, (rep ^ j) * cols, cols, 0)
        ups.append(swap(u, "rep", j))
        downs.append(swap(d, "rep", j))
    up, down = gather_weights(w_up, w_down, ups, downs)

    mine = dict(hidden_in=hidden_in, cotangent=cotangent)
    theirs = {}
    for plane, own in (("near", near), ("far", far), ("across", across)):
        x = swap(own, "fs", 1)
        y = swap(own, "fs", 2)
        f = swap(x[:part], "fs", 2)
        g = swap(y[part:], "fs", 1)
        for kind, value in zip("oxyfg", (own, x, y, f, g)):
            mine[plane + kind] = value
            theirs[plane + kind] = swap(value, "tp", 1)

    def add(a, b):
        return (a.astype(F32) + b.astype(F32)).astype(BF16)

    def hidden_units(hidden_rows, cot_rows):
        active = jnp.maximum(jnp.dot(hidden_rows, up, preferred_element_type=F32), 0.0)
        back_grad = jnp.dot(cot_rows, down.T, preferred_element_type=F32)
        return (active * active).astype(BF16), (2.0 * active * back_grad).astype(BF16)

    def between_cores(slopes):
        sent = contract_last(slopes[tokens:], up).astype(BF16)
        got = swap(sent, "tp", 1)
        kept = contract_last(slopes[:tokens], up) + got.astype(F32)
        return kept.astype(BF16).reshape(2, n_fs, part, width)

    def over_places(kept):
        left, right = kept[..., :half], kept[..., half:]
        got_left = swap(left[:, 1::2], "fs", 1)
        got_right = swap(right[:, 2:], "fs", 2)
        left, right = add(left[:, ::2], got_left), add(right[:, :2], got_right)
        got_left = swap(left[:, 1], "fs", 2)
        got_right = swap(right[:, 1], "fs", 1)
        return jnp.concatenate([add(left[:, 0], got_left), add(right[:, 0], got_right)], -1)

    h_even, c_even = gather_rows(mine, theirs, ("far", "own"))
    h_odd, c_odd = gather_rows(mine, theirs, ("near", "across"))
    hidden_odd, slopes_odd = hidden_units(h_odd, c_odd)
    kept_odd = between_cores(slopes_odd)
    hidden_even, slopes_even = hidden_units(h_even, c_even)
    kept_even = between_cores(slopes_even)
    odd = over_places(kept_odd)
    even = over_places(kept_even)
    got = swap(odd, "rep", 1)
    own_sum = even[1].astype(F32) + got[0].astype(F32)
    far_sum = add(even[0], got[1])
    final = (own_sum + swap(far_sum, "rep", 2).astype(F32)).astype(BF16)
    blocks = [final] + [swap(final, "fs", b) for b in (1, 2, 3)]
    ours = jnp.zeros((side, width), BF16)
    for b, value in enumerate(blocks):
        ours = lax.dynamic_update_slice_in_dim(ours, value, (fs ^ b) * part, 0)
    others = swap(ours, "tp", 1)
    input_grad = jnp.zeros((tokens, width), BF16)
    input_grad = lax.dynamic_update_slice_in_dim(input_grad, ours, tp * side, 0)
    input_grad = lax.dynamic_update_slice_in_dim(input_grad, others, (1 - tp) * side, 0)

    up_own = (contract_first(h_odd, slopes_odd) + contract_first(h_even, slopes_even)).astype(BF16)
    down_own = (contract_first(hidden_odd, c_odd) + contract_first(hidden_even, c_even)).astype(BF16)
    ups, downs = [], []
    for j in range(n_rep):
        u = lax.dynamic_slice_in_dim(up_own, (rep ^ j) * shard, shard, 0)
        d = lax.dynamic_slice_in_dim(down_own, (rep ^ j) * shard, shard, 1)
        if j:
            u, d = swap(u, "rep", j), swap(d, "rep", j)
        ups.append(u)
        downs.append(d)
    ups, downs, final = lax.optimization_barrier((ups, downs, final))
    up_grad = jnp.zeros((shard, cols * n_rep), F32)
    down_grad = jnp.zeros((cols * n_rep, shard), F32)
    for j in range(n_rep):
        up_grad = lax.dynamic_update_slice_in_dim(up_grad, ups[j].astype(F32), (rep ^ j) * cols, 1)
        down_grad = lax.dynamic_update_slice_in_dim(down_grad, downs[j].astype(F32), (rep ^ j) * cols, 0)
    return input_grad, up_grad, down_grad


def on_device(hidden_in, cotangent, w_up, w_down):
    sizes = tuple(lax.axis_size(a) for a in ("rep", "fs", "tp"))
    gathered = 2 * hidden_in.size * sizes[0] * hidden_in.dtype.itemsize
    fits = sizes == (4, 4, 2) and gathered <= GATHER_BUDGET
    plan = gathered_tokens if fits else gathered_weights
    return plan(hidden_in, cotangent, w_up, w_down)


def solution(mesh):
    return jax.shard_map(
        on_device,
        mesh=mesh,
        in_specs=(P("rep", None), P("rep", None), P("rep", ("fs", "tp")), P(("fs", "tp"), "rep")),
        out_specs=(P("rep", None), P("rep", ("fs", "tp")), P(("fs", "tp"), "rep")),
        check_vma=False,
    )
```

```python
import functools

import jax
import jax.numpy as jnp
from jax import lax
from jax.experimental import pallas as pl
from jax.experimental.pallas import tpu as pltpu
from jax.sharding import PartitionSpec as P

BF16 = jnp.bfloat16
F32 = jnp.float32
GATHER_BUDGET = 20 << 20


def contract_last(left, right):
    return lax.dot_general(
        left, right, (((1,), (1,)), ((), ())), preferred_element_type=F32
    )


def contract_first(left, right):
    return lax.dot_general(
        left, right, (((0,), (0,)), ((), ())), preferred_element_type=F32
    )


def swap(value, axis, offset):
    size = lax.axis_size(axis)
    return lax.ppermute(value, axis, [(i, i ^ offset) for i in range(size)])


def gathered_weights(hidden_in, cotangent, w_up, w_down):
    up_full = lax.all_gather(w_up, "rep", axis=0, tiled=True)
    back_grad = contract_last(cotangent, lax.all_gather(w_down, "rep", axis=1, tiled=True))
    preact = jnp.dot(hidden_in, up_full, preferred_element_type=F32)
    active = jnp.maximum(preact, 0.0)
    hidden = (active * active).astype(BF16)
    slopes = (2.0 * active * back_grad).astype(BF16)
    grad_upper = lax.psum_scatter(
        contract_first(hidden_in, slopes).astype(BF16), "rep", scatter_dimension=0, tiled=True
    ).astype(F32)
    lower_rows = lax.psum_scatter(
        contract_first(cotangent, hidden).astype(BF16), "rep", scatter_dimension=0, tiled=True
    ).astype(F32)
    partial_sum = contract_last(slopes, up_full).astype(BF16)
    input_grad = lax.psum(partial_sum, ("fs", "tp"))
    return input_grad, grad_upper, lower_rows.T


def finish(ref, sem):
    pltpu.make_async_copy(ref, ref, sem).wait()


def gather_kernel(mine, theirs, planes, *refs):
    ins = (dict(zip(mine, refs)), dict(zip(theirs, refs[len(mine) :])))
    outs = refs[len(mine) + len(theirs) :][:2]
    sems = refs[-1]
    fs, tp = lax.axis_index("fs"), lax.axis_index("tp")
    part = outs[0].shape[0] // (8 * len(planes))
    for which, name in enumerate(("hidden_in", "cotangent")):
        for core in range(2):
            for k, plane in enumerate(planes):
                for b in range(4):
                    if plane == "own":
                        at = pl.multiple_of(((tp ^ core) * 4 + (fs ^ b)) * part, part)
                        src = ins[0][name].at[pl.ds(at, part), :]
                    elif b < 3 and plane == "near":
                        src = ins[core][plane + "oxy"[b] + "hc"[which]]
                    elif b < 3:
                        src = ins[core][plane + "oxy"[b]].at[which * part : (which + 1) * part, :]
                    else:
                        src = ins[core][plane + "fg"[which]]
                    to = pl.ds(((core * len(planes) + k) * 4 + b) * part, part)
                    pltpu.make_async_copy(src, outs[which].at[to, :], sems.at[which]).start()
    finish(outs[0], sems.at[0])
    finish(outs[1], sems.at[1])


def cut(value, at, count, dim):
    starts = [at if d == dim else 0 for d in range(2)]
    sizes = [count if d == dim else n for d, n in enumerate(value.shape)]
    return lax.dynamic_slice(value, starts, sizes, allow_negative_indices=False)


def put(into, value, at, dim):
    starts = [at if d == dim else 0 for d in range(2)]
    return lax.dynamic_update_slice(into, value, starts, allow_negative_indices=False)


def theirs_of(pieces, planes):
    return [name for name in pieces if name.startswith(planes)]


def gather_rows(mine, theirs, planes):
    tokens, width = mine["hidden_in"].shape
    pieces = list(theirs_of(theirs, planes))
    whole = ["hidden_in", "cotangent"]
    any_space = pl.BlockSpec(memory_space=pl.ANY)
    out = pltpu.VMEM((len(planes) * tokens, width), BF16)
    return pl.pallas_call(
        functools.partial(gather_kernel, whole + pieces, pieces, planes),
        out_shape=[out, out],
        in_specs=[pl.BlockSpec(memory_space=pltpu.HBM)] * 2 + [any_space] * (2 * len(pieces)),
        out_specs=[any_space] * 2,
        scratch_shapes=[pltpu.SemaphoreType.DMA((2,))],
        cost_estimate=pl.CostEstimate(flops=4_000_000_000, bytes_accessed=4 * tokens * width * len(planes), transcendentals=0),
        compiler_params=pltpu.CompilerParams(vmem_limit_bytes=1 << 20),
    )(*[mine[k] for k in whole + pieces], *[theirs[k] for k in pieces])


def weights_kernel(w_up, w_down, *refs):
    ups, downs, (up, down, sems) = refs[:3], refs[3:6], refs[6:]
    rep = lax.axis_index("rep")
    shard, cols = w_up.shape[0], up.shape[1]
    for j in range(4):
        at = pl.multiple_of((rep ^ j) * shard, shard)
        mine = pl.multiple_of(rep * cols, cols)
        u = ups[j - 1] if j else w_up.at[:, pl.ds(mine, cols)]
        d = downs[j - 1] if j else w_down.at[pl.ds(mine, cols), :]
        pltpu.make_async_copy(u, up.at[pl.ds(at, shard), :], sems.at[0]).start()
        pltpu.make_async_copy(d, down.at[:, pl.ds(at, shard)], sems.at[1]).start()
    finish(up, sems.at[0])
    finish(down, sems.at[1])


def gather_weights(w_up, w_down, ups, downs):
    (shard, cols), width = ups[0].shape, w_down.shape[1] * 4
    any_space = pl.BlockSpec(memory_space=pl.ANY)
    return pl.pallas_call(
        weights_kernel,
        out_shape=[pltpu.VMEM((width, cols), BF16), pltpu.VMEM((cols, width), BF16)],
        in_specs=[pl.BlockSpec(memory_space=pltpu.HBM)] * 2 + [any_space] * 6,
        out_specs=[any_space] * 2,
        scratch_shapes=[pltpu.SemaphoreType.DMA((2,))],
        cost_estimate=pl.CostEstimate(flops=1_000_000_000, bytes_accessed=4 * width * cols, transcendentals=0),
        compiler_params=pltpu.CompilerParams(vmem_limit_bytes=1 << 20),
        name="weights",
    )(w_up, w_down, *ups, *downs)


def gathered_tokens(hidden_in, cotangent, w_up, w_down):
    n_rep, n_fs = lax.axis_size("rep"), lax.axis_size("fs")
    rep, fs, tp = (lax.axis_index(a) for a in ("rep", "fs", "tp"))
    tokens, width = hidden_in.shape
    side = tokens // 2
    part = side // n_fs
    half = width // 2
    shard = w_up.shape[0]
    cols = w_up.shape[1] // n_rep

    at_shard = [(rep ^ j) * shard for j in range(n_rep)]
    at_cols = [(rep ^ j) * cols for j in range(n_rep)]
    at_block = [(fs ^ b) * part for b in range(n_fs)]
    at_side = [tp * side, (1 - tp) * side]

    at_own = at_side[0] + at_block[0]
    own_h, own_c = cut(hidden_in, at_own, part, 0), cut(cotangent, at_own, part, 0)
    near_h = swap(own_h, "rep", 1)
    near_c = swap(own_c, "rep", 1)
    far = swap(jnp.concatenate([own_h, own_c], 0), "rep", 2)
    across = swap(far, "rep", 1)

    ups, downs = [], []
    for j in range(1, n_rep):
        u = cut(w_up, at_cols[j], cols, 1)
        d = cut(w_down, at_cols[j], cols, 0)
        ups.append(swap(u, "rep", j))
        downs.append(swap(d, "rep", j))
    near_h, at_shard = lax.optimization_barrier((near_h, at_shard))
    up, down = gather_weights(w_up, w_down, ups, downs)

    mine = dict(hidden_in=hidden_in, cotangent=cotangent)
    theirs = {}

    def keep(name, value):
        mine[name] = value
        theirs[name] = swap(value, "tp", 1)

    for own, kind in ((near_h, "h"), (near_c, "c")):
        x = swap(own, "fs", 1)
        y = swap(own, "fs", 2)
        f = swap(x if kind == "h" else y, "fs", 2 if kind == "h" else 1)
        for name, value in (("o", own), ("x", x), ("y", y)):
            keep("near" + name + kind, value)
        keep("near" + ("f" if kind == "h" else "g"), f)
    for plane, own in (("far", far), ("across", across)):
        x = swap(own, "fs", 1)
        y = swap(own, "fs", 2)
        f = swap(x[:part], "fs", 2)
        g = swap(y[part:], "fs", 1)
        for kind, value in zip("oxyfg", (own, x, y, f, g)):
            keep(plane + kind, value)

    def add(a, b):
        return (a.astype(F32) + b.astype(F32)).astype(BF16)

    def hidden_units(hidden_rows, cot_rows):
        active = jnp.maximum(jnp.dot(hidden_rows, up, preferred_element_type=F32), 0.0)
        back_grad = jnp.dot(cot_rows, down.T, preferred_element_type=F32)
        return (active * active).astype(BF16), (2.0 * active * back_grad).astype(BF16)

    def between_cores(slopes):
        sent = contract_last(slopes[tokens:], up).astype(BF16)
        got = swap(sent, "tp", 1)
        kept = contract_last(slopes[:tokens], up) + got.astype(F32)
        return kept.astype(BF16).reshape(2, n_fs, part, width)

    def over_places(kept):
        left, right = kept[..., :half], kept[..., half:]
        got_left = swap(left[:, 1::2], "fs", 1)
        got_right = swap(right[:, 2:], "fs", 2)
        left, right = add(left[:, ::2], got_left), add(right[:, :2], got_right)
        got_left = swap(left[:, 1], "fs", 2)
        got_right = swap(right[:, 1], "fs", 1)
        return jnp.concatenate([add(left[:, 0], got_left), add(right[:, 0], got_right)], -1)

    h_first, c_first = gather_rows(mine, theirs, ("near", "far"))
    h_last, c_last = gather_rows(mine, theirs, ("across", "own"))
    hidden_first, slopes_first = hidden_units(h_first, c_first)
    kept_first = between_cores(slopes_first)
    hidden_last, slopes_last = hidden_units(h_last, c_last)
    kept_last = between_cores(slopes_last)
    first = over_places(kept_first)
    last = over_places(kept_last)
    got = swap(first, "rep", 1)
    own_sum = last[1].astype(F32) + got[0].astype(F32)
    across_sum = add(last[0], got[1])
    final = (own_sum + swap(across_sum, "rep", 3).astype(F32)).astype(BF16)
    blocks = [final] + [swap(final, "fs", b) for b in (1, 2, 3)]
    ours = jnp.zeros((side, width), BF16)
    for b, value in enumerate(blocks):
        ours = put(ours, value, at_block[b], 0)
    others = swap(ours, "tp", 1)
    input_grad = jnp.zeros((tokens, width), BF16)
    input_grad = put(put(input_grad, ours, at_side[0], 0), others, at_side[1], 0)

    up_own = (contract_first(h_first, slopes_first) + contract_first(h_last, slopes_last)).astype(BF16)
    down_own = (contract_first(hidden_first, c_first) + contract_first(hidden_last, c_last)).astype(BF16)
    ups, downs = [], []
    for j in range(n_rep):
        u = cut(up_own, at_shard[j], shard, 0)
        d = cut(down_own, at_shard[j], shard, 1)
        if j:
            u, d = swap(u, "rep", j), swap(d, "rep", j)
        ups.append(u)
        downs.append(d)
    ups, downs, final = lax.optimization_barrier((ups, downs, final))
    up_grad = jnp.zeros((shard, cols * n_rep), F32)
    down_grad = jnp.zeros((cols * n_rep, shard), F32)
    for j in range(n_rep):
        up_grad = put(up_grad, ups[j].astype(F32), at_cols[j], 1)
        down_grad = put(down_grad, downs[j].astype(F32), at_cols[j], 0)
    return input_grad, up_grad, down_grad


def on_device(hidden_in, cotangent, w_up, w_down):
    sizes = tuple(lax.axis_size(a) for a in ("rep", "fs", "tp"))
    gathered = 2 * hidden_in.size * sizes[0] * hidden_in.dtype.itemsize
    fits = sizes == (4, 4, 2) and gathered <= GATHER_BUDGET
    plan = gathered_tokens if fits else gathered_weights
    return plan(hidden_in, cotangent, w_up, w_down)


def solution(mesh):
    return jax.shard_map(
        on_device,
        mesh=mesh,
        in_specs=(P("rep", None), P("rep", None), P("rep", ("fs", "tp")), P(("fs", "tp"), "rep")),
        out_specs=(P("rep", None), P("rep", ("fs", "tp")), P(("fs", "tp"), "rep")),
        check_vma=False,
    )
```

```python
import functools

import jax
import jax.numpy as jnp
from jax import lax
from jax.experimental import pallas as pl
from jax.experimental.pallas import tpu as pltpu
from jax.sharding import PartitionSpec as P

BF16 = jnp.bfloat16
F32 = jnp.float32
GATHER_BUDGET = 20 << 20


def contract_last(left, right):
    return lax.dot_general(
        left, right, (((1,), (1,)), ((), ())), preferred_element_type=F32
    )


def contract_first(left, right):
    return lax.dot_general(
        left, right, (((0,), (0,)), ((), ())), preferred_element_type=F32
    )


def swap(value, axis, offset):
    size = lax.axis_size(axis)
    return lax.ppermute(value, axis, [(i, i ^ offset) for i in range(size)])


def gathered_weights(hidden_in, cotangent, w_up, w_down):
    up_full = lax.all_gather(w_up, "rep", axis=0, tiled=True)
    back_grad = contract_last(cotangent, lax.all_gather(w_down, "rep", axis=1, tiled=True))
    preact = jnp.dot(hidden_in, up_full, preferred_element_type=F32)
    active = jnp.maximum(preact, 0.0)
    hidden = (active * active).astype(BF16)
    slopes = (2.0 * active * back_grad).astype(BF16)
    grad_upper = lax.psum_scatter(
        contract_first(hidden_in, slopes).astype(BF16), "rep", scatter_dimension=0, tiled=True
    ).astype(F32)
    lower_rows = lax.psum_scatter(
        contract_first(cotangent, hidden).astype(BF16), "rep", scatter_dimension=0, tiled=True
    ).astype(F32)
    partial_sum = contract_last(slopes, up_full).astype(BF16)
    input_grad = lax.psum(partial_sum, ("fs", "tp"))
    return input_grad, grad_upper, lower_rows.T


def finish(ref, sem):
    pltpu.make_async_copy(ref, ref, sem).wait()


def gather_kernel(mine, theirs, planes, *refs):
    ins = (dict(zip(mine, refs)), dict(zip(theirs, refs[len(mine) :])))
    outs = refs[len(mine) + len(theirs) :][:2]
    sems = refs[-1]
    fs, tp = lax.axis_index("fs"), lax.axis_index("tp")
    part = outs[0].shape[0] // (8 * len(planes))
    for which, name in enumerate(("hidden_in", "cotangent")):
        for core in range(2):
            for k, plane in enumerate(planes):
                for b in range(4):
                    if plane == "own":
                        at = pl.multiple_of(((tp ^ core) * 4 + (fs ^ b)) * part, part)
                        src = ins[0][name].at[pl.ds(at, part), :]
                    elif b < 3 and plane == "near":
                        src = ins[core][plane + "oxy"[b] + "hc"[which]]
                    elif b < 3:
                        src = ins[core][plane + "oxy"[b]].at[which * part : (which + 1) * part, :]
                    else:
                        src = ins[core][plane + "fg"[which]]
                    to = pl.ds(((core * len(planes) + k) * 4 + b) * part, part)
                    pltpu.make_async_copy(src, outs[which].at[to, :], sems.at[which]).start()
    finish(outs[0], sems.at[0])
    finish(outs[1], sems.at[1])


def cut(value, at, count, dim):
    starts = [at if d == dim else 0 for d in range(2)]
    sizes = [count if d == dim else n for d, n in enumerate(value.shape)]
    return lax.dynamic_slice(value, starts, sizes, allow_negative_indices=False)


def put(into, value, at, dim):
    starts = [at if d == dim else 0 for d in range(2)]
    return lax.dynamic_update_slice(into, value, starts, allow_negative_indices=False)


def theirs_of(pieces, planes):
    return [name for name in pieces if name.startswith(planes)]


def gather_rows(mine, theirs, planes):
    tokens, width = mine["hidden_in"].shape
    pieces = list(theirs_of(theirs, planes))
    whole = ["hidden_in", "cotangent"]
    any_space = pl.BlockSpec(memory_space=pl.ANY)
    out = pltpu.VMEM((len(planes) * tokens, width), BF16)
    return pl.pallas_call(
        functools.partial(gather_kernel, whole + pieces, pieces, planes),
        out_shape=[out, out],
        in_specs=[pl.BlockSpec(memory_space=pltpu.HBM)] * 2 + [any_space] * (2 * len(pieces)),
        out_specs=[any_space] * 2,
        scratch_shapes=[pltpu.SemaphoreType.DMA((2,))],
        cost_estimate=pl.CostEstimate(flops=4_000_000_000, bytes_accessed=4 * tokens * width * len(planes), transcendentals=0),
        compiler_params=pltpu.CompilerParams(vmem_limit_bytes=1 << 20),
    )(*[mine[k] for k in whole + pieces], *[theirs[k] for k in pieces])


def weight_kernel(dim, own, *refs):
    others, (out, sem) = refs[:3], refs[3:]
    rep = lax.axis_index("rep")
    shard, cols = own.shape[dim], out.shape[1 - dim]
    for j in range(4):
        at = pl.ds(pl.multiple_of((rep ^ j) * shard, shard), shard)
        mine = pl.ds(pl.multiple_of(rep * cols, cols), cols)
        to = out.at[at, :] if dim == 0 else out.at[:, at]
        src = others[j - 1] if j else own.at[:, mine] if dim == 0 else own.at[mine, :]
        pltpu.make_async_copy(src, to, sem).start()
    finish(out, sem)


def gather_weight(own, others, dim):
    size = [n * 4 if d == dim else n for d, n in enumerate(others[0].shape)]
    any_space = pl.BlockSpec(memory_space=pl.ANY)
    return pl.pallas_call(
        functools.partial(weight_kernel, dim),
        out_shape=pltpu.VMEM(tuple(size), BF16),
        in_specs=[pl.BlockSpec(memory_space=pltpu.HBM)] + [any_space] * 3,
        out_specs=any_space,
        scratch_shapes=[pltpu.SemaphoreType.DMA],
        cost_estimate=pl.CostEstimate(flops=1_000_000_000, bytes_accessed=2 * size[0] * size[1], transcendentals=0),
        compiler_params=pltpu.CompilerParams(vmem_limit_bytes=1 << 20),
        name="down" if dim else "up",
    )(own, *others)


def gathered_tokens(hidden_in, cotangent, w_up, w_down):
    n_rep, n_fs = lax.axis_size("rep"), lax.axis_size("fs")
    rep, fs, tp = (lax.axis_index(a) for a in ("rep", "fs", "tp"))
    tokens, width = hidden_in.shape
    side = tokens // 2
    part = side // n_fs
    half = width // 2
    shard = w_up.shape[0]
    cols = w_up.shape[1] // n_rep

    at_shard = [(rep ^ j) * shard for j in range(n_rep)]
    at_cols = [(rep ^ j) * cols for j in range(n_rep)]
    at_block = [(fs ^ b) * part for b in range(n_fs)]
    at_side = [tp * side, (1 - tp) * side]

    at_own = at_side[0] + at_block[0]
    own_h, own_c = cut(hidden_in, at_own, part, 0), cut(cotangent, at_own, part, 0)
    near_h = swap(own_h, "rep", 1)
    near_c = swap(own_c, "rep", 1)
    far = swap(jnp.concatenate([own_h, own_c], 0), "rep", 2)
    across = swap(far, "rep", 1)

    ups, downs = [], []
    for j in range(1, n_rep):
        u = cut(w_up, at_cols[j], cols, 1)
        d = cut(w_down, at_cols[j], cols, 0)
        ups.append(swap(u, "rep", j))
        downs.append(swap(d, "rep", j))
    near_h, at_shard = lax.optimization_barrier((near_h, at_shard))
    up = gather_weight(w_up, ups, 0)
    down = gather_weight(w_down, downs, 1)

    mine = dict(hidden_in=hidden_in, cotangent=cotangent)
    theirs = {}

    def keep(name, value):
        mine[name] = value
        theirs[name] = swap(value, "tp", 1)

    for own, kind in ((near_h, "h"), (near_c, "c")):
        x = swap(own, "fs", 1)
        y = swap(own, "fs", 2)
        f = swap(x if kind == "h" else y, "fs", 2 if kind == "h" else 1)
        for name, value in (("o", own), ("x", x), ("y", y)):
            keep("near" + name + kind, value)
        keep("near" + ("f" if kind == "h" else "g"), f)
    for plane, own in (("far", far), ("across", across)):
        x = swap(own, "fs", 1)
        y = swap(own, "fs", 2)
        f = swap(x[:part], "fs", 2)
        g = swap(y[part:], "fs", 1)
        for kind, value in zip("oxyfg", (own, x, y, f, g)):
            keep(plane + kind, value)

    def add(a, b):
        return (a.astype(F32) + b.astype(F32)).astype(BF16)

    def active_units(rows):
        return jnp.maximum(jnp.dot(rows, up, preferred_element_type=F32), 0.0)

    def slopes_of(active, rows):
        return (2.0 * active * jnp.dot(rows, down.T, preferred_element_type=F32)).astype(BF16)

    def between_cores(slopes):
        sent = contract_last(slopes[tokens:], up).astype(BF16)
        got = swap(sent, "tp", 1)
        kept = contract_last(slopes[:tokens], up) + got.astype(F32)
        return kept.astype(BF16).reshape(2, n_fs, part, width)

    def over_places(kept):
        left, right = kept[..., :half], kept[..., half:]
        got_left = swap(left[:, 1::2], "fs", 1)
        got_right = swap(right[:, 2:], "fs", 2)
        left, right = add(left[:, ::2], got_left), add(right[:, :2], got_right)
        got_left = swap(left[:, 1], "fs", 2)
        got_right = swap(right[:, 1], "fs", 1)
        return jnp.concatenate([add(left[:, 0], got_left), add(right[:, 0], got_right)], -1)

    h_first, c_first = gather_rows(mine, theirs, ("near", "far"))
    h_last, c_last = gather_rows(mine, theirs, ("across", "own"))
    active_first = active_units(h_first)
    active_last = active_units(h_last)
    hidden_first = (active_first * active_first).astype(BF16)
    hidden_last = (active_last * active_last).astype(BF16)
    slopes_first = slopes_of(active_first, c_first)
    kept_first = between_cores(slopes_first)
    slopes_last = slopes_of(active_last, c_last)
    kept_last = between_cores(slopes_last)
    first = over_places(kept_first)
    last = over_places(kept_last)
    got = swap(first, "rep", 1)
    own_sum = last[1].astype(F32) + got[0].astype(F32)
    across_sum = add(last[0], got[1])
    final = (own_sum + swap(across_sum, "rep", 3).astype(F32)).astype(BF16)
    blocks = [final] + [swap(final, "fs", b) for b in (1, 2, 3)]
    ours = jnp.zeros((side, width), BF16)
    for b, value in enumerate(blocks):
        ours = put(ours, value, at_block[b], 0)
    others = swap(ours, "tp", 1)
    input_grad = jnp.zeros((tokens, width), BF16)
    input_grad = put(put(input_grad, ours, at_side[0], 0), others, at_side[1], 0)

    up_own = (contract_first(h_first, slopes_first) + contract_first(h_last, slopes_last)).astype(BF16)
    down_own = (contract_first(hidden_first, c_first) + contract_first(hidden_last, c_last)).astype(BF16)
    ups, downs = [], []
    for j in range(n_rep):
        u = cut(up_own, at_shard[j], shard, 0)
        d = cut(down_own, at_shard[j], shard, 1)
        if j:
            u, d = swap(u, "rep", j), swap(d, "rep", j)
        ups.append(u)
        downs.append(d)
    ups[0], ups[2], ups[3], downs[0], downs[2], downs[3], final = lax.optimization_barrier(
        (ups[0], ups[2], ups[3], downs[0], downs[2], downs[3], final)
    )
    ups[1], downs[1], ours = lax.optimization_barrier((ups[1], downs[1], ours))
    up_grad = jnp.zeros((shard, cols * n_rep), F32)
    down_grad = jnp.zeros((cols * n_rep, shard), F32)
    for j in (0, 2, 3, 1):
        up_grad = put(up_grad, ups[j].astype(F32), at_cols[j], 1)
        down_grad = put(down_grad, downs[j].astype(F32), at_cols[j], 0)
    return input_grad, up_grad, down_grad


def on_device(hidden_in, cotangent, w_up, w_down):
    sizes = tuple(lax.axis_size(a) for a in ("rep", "fs", "tp"))
    gathered = 2 * hidden_in.size * sizes[0] * hidden_in.dtype.itemsize
    fits = sizes == (4, 4, 2) and gathered <= GATHER_BUDGET
    plan = gathered_tokens if fits else gathered_weights
    return plan(hidden_in, cotangent, w_up, w_down)


def solution(mesh):
    return jax.shard_map(
        on_device,
        mesh=mesh,
        in_specs=(P("rep", None), P("rep", None), P("rep", ("fs", "tp")), P(("fs", "tp"), "rep")),
        out_specs=(P("rep", None), P("rep", ("fs", "tp")), P(("fs", "tp"), "rep")),
        check_vma=False,
    )
```

```python
import functools

import jax
import jax.numpy as jnp
from jax import lax
from jax.experimental import pallas as pl
from jax.experimental.pallas import tpu as pltpu
from jax.sharding import PartitionSpec as P

BF16 = jnp.bfloat16
F32 = jnp.float32
GATHER_BUDGET = 20 << 20


def contract_last(left, right):
    return lax.dot_general(
        left, right, (((1,), (1,)), ((), ())), preferred_element_type=F32
    )


def contract_first(left, right):
    return lax.dot_general(
        left, right, (((0,), (0,)), ((), ())), preferred_element_type=F32
    )


def swap(value, axis, offset):
    size = lax.axis_size(axis)
    return lax.ppermute(value, axis, [(i, i ^ offset) for i in range(size)])


def gathered_weights(hidden_in, cotangent, w_up, w_down):
    up_full = lax.all_gather(w_up, "rep", axis=0, tiled=True)
    back_grad = contract_last(cotangent, lax.all_gather(w_down, "rep", axis=1, tiled=True))
    preact = jnp.dot(hidden_in, up_full, preferred_element_type=F32)
    active = jnp.maximum(preact, 0.0)
    hidden = (active * active).astype(BF16)
    slopes = (2.0 * active * back_grad).astype(BF16)
    grad_upper = lax.psum_scatter(
        contract_first(hidden_in, slopes).astype(BF16), "rep", scatter_dimension=0, tiled=True
    ).astype(F32)
    lower_rows = lax.psum_scatter(
        contract_first(cotangent, hidden).astype(BF16), "rep", scatter_dimension=0, tiled=True
    ).astype(F32)
    partial_sum = contract_last(slopes, up_full).astype(BF16)
    input_grad = lax.psum(partial_sum, ("fs", "tp"))
    return input_grad, grad_upper, lower_rows.T


def finish(ref, sem):
    pltpu.make_async_copy(ref, ref, sem).wait()


def gather_kernel(mine, theirs, planes, *refs):
    ins = (dict(zip(mine, refs)), dict(zip(theirs, refs[len(mine) :])))
    outs = refs[len(mine) + len(theirs) :][:2]
    sems = refs[-1]
    fs, tp = lax.axis_index("fs"), lax.axis_index("tp")
    part = outs[0].shape[0] // (8 * len(planes))
    for which, name in enumerate(("hidden_in", "cotangent")):
        for core in range(2):
            for k, plane in enumerate(planes):
                for b in range(4):
                    if plane == "own":
                        at = pl.multiple_of(((tp ^ core) * 4 + (fs ^ b)) * part, part)
                        src = ins[0][name].at[pl.ds(at, part), :]
                    elif b < 3 and plane == "near":
                        src = ins[core][plane + "oxy"[b] + "hc"[which]]
                    elif b < 3:
                        src = ins[core][plane + "oxy"[b]].at[which * part : (which + 1) * part, :]
                    else:
                        src = ins[core][plane + "fg"[which]]
                    to = pl.ds(((core * len(planes) + k) * 4 + b) * part, part)
                    pltpu.make_async_copy(src, outs[which].at[to, :], sems.at[which]).start()
    finish(outs[0], sems.at[0])
    finish(outs[1], sems.at[1])


def cut(value, at, count, dim):
    starts = [at if d == dim else 0 for d in range(2)]
    sizes = [count if d == dim else n for d, n in enumerate(value.shape)]
    return lax.dynamic_slice(value, starts, sizes, allow_negative_indices=False)


def put(into, value, at, dim):
    starts = [at if d == dim else 0 for d in range(2)]
    return lax.dynamic_update_slice(into, value, starts, allow_negative_indices=False)


def theirs_of(pieces, planes):
    return [name for name in pieces if name.startswith(planes)]


def gather_rows(mine, theirs, planes):
    tokens, width = mine["hidden_in"].shape
    pieces = list(theirs_of(theirs, planes))
    whole = ["hidden_in", "cotangent"]
    any_space = pl.BlockSpec(memory_space=pl.ANY)
    out = pltpu.VMEM((len(planes) * tokens, width), BF16)
    return pl.pallas_call(
        functools.partial(gather_kernel, whole + pieces, pieces, planes),
        out_shape=[out, out],
        in_specs=[pl.BlockSpec(memory_space=pltpu.HBM)] * 2 + [any_space] * (2 * len(pieces)),
        out_specs=[any_space] * 2,
        scratch_shapes=[pltpu.SemaphoreType.DMA((2,))],
        cost_estimate=pl.CostEstimate(flops=4_000_000_000, bytes_accessed=4 * tokens * width * len(planes), transcendentals=0),
        compiler_params=pltpu.CompilerParams(vmem_limit_bytes=1 << 20),
    )(*[mine[k] for k in whole + pieces], *[theirs[k] for k in pieces])


def weight_kernel(dim, own, *refs):
    others, (out, sem) = refs[:3], refs[3:]
    rep = lax.axis_index("rep")
    shard, cols = own.shape[dim], out.shape[1 - dim]
    for j in range(4):
        at = pl.ds(pl.multiple_of((rep ^ j) * shard, shard), shard)
        mine = pl.ds(pl.multiple_of(rep * cols, cols), cols)
        to = out.at[at, :] if dim == 0 else out.at[:, at]
        src = others[j - 1] if j else own.at[:, mine] if dim == 0 else own.at[mine, :]
        pltpu.make_async_copy(src, to, sem).start()
    finish(out, sem)


def gather_weight(own, others, dim):
    size = [n * 4 if d == dim else n for d, n in enumerate(others[0].shape)]
    any_space = pl.BlockSpec(memory_space=pl.ANY)
    return pl.pallas_call(
        functools.partial(weight_kernel, dim),
        out_shape=pltpu.VMEM(tuple(size), BF16),
        in_specs=[pl.BlockSpec(memory_space=pltpu.HBM)] + [any_space] * 3,
        out_specs=any_space,
        scratch_shapes=[pltpu.SemaphoreType.DMA],
        cost_estimate=pl.CostEstimate(flops=1_000_000_000, bytes_accessed=2 * size[0] * size[1], transcendentals=0),
        compiler_params=pltpu.CompilerParams(vmem_limit_bytes=1 << 20),
        name="down" if dim else "up",
    )(own, *others)


def gathered_tokens(hidden_in, cotangent, w_up, w_down):
    n_rep, n_fs = lax.axis_size("rep"), lax.axis_size("fs")
    rep, fs, tp = (lax.axis_index(a) for a in ("rep", "fs", "tp"))
    tokens, width = hidden_in.shape
    side = tokens // 2
    part = side // n_fs
    half = width // 2
    shard = w_up.shape[0]
    cols = w_up.shape[1] // n_rep

    at_shard = [(rep ^ j) * shard for j in range(n_rep)]
    at_cols = [(rep ^ j) * cols for j in range(n_rep)]
    at_block = [(fs ^ b) * part for b in range(n_fs)]
    at_side = [tp * side, (1 - tp) * side]

    at_own = at_side[0] + at_block[0]
    own_h, own_c = cut(hidden_in, at_own, part, 0), cut(cotangent, at_own, part, 0)
    near_h = swap(own_h, "rep", 1)
    near_c = swap(own_c, "rep", 1)
    far = swap(jnp.concatenate([own_h, own_c], 0), "rep", 2)
    across = swap(far, "rep", 1)

    ups, downs = [], []
    for j in range(1, n_rep):
        u = cut(w_up, at_cols[j], cols, 1)
        d = cut(w_down, at_cols[j], cols, 0)
        ups.append(swap(u, "rep", j))
        downs.append(swap(d, "rep", j))
    near_h, at_shard = lax.optimization_barrier((near_h, at_shard))
    up = gather_weight(w_up, ups, 0)
    down = gather_weight(w_down, downs, 1)

    mine = dict(hidden_in=hidden_in, cotangent=cotangent)
    theirs = {}

    def keep(name, value):
        mine[name] = value
        theirs[name] = swap(value, "tp", 1)

    for own, kind in ((near_h, "h"), (near_c, "c")):
        x = swap(own, "fs", 1)
        y = swap(own, "fs", 2)
        f = swap(x if kind == "h" else y, "fs", 2 if kind == "h" else 1)
        for name, value in (("o", own), ("x", x), ("y", y)):
            keep("near" + name + kind, value)
        keep("near" + ("f" if kind == "h" else "g"), f)
    for plane, own in (("far", far), ("across", across)):
        x = swap(own, "fs", 1)
        y = swap(own, "fs", 2)
        f = swap(x[:part], "fs", 2)
        g = swap(y[part:], "fs", 1)
        for kind, value in zip("oxyfg", (own, x, y, f, g)):
            keep(plane + kind, value)

    def add(a, b):
        return (a.astype(F32) + b.astype(F32)).astype(BF16)

    def active_units(rows):
        return jnp.maximum(jnp.dot(rows, up, preferred_element_type=F32), 0.0)

    def slopes_of(active, rows):
        return (2.0 * active * jnp.dot(rows, down.T, preferred_element_type=F32)).astype(BF16)

    def between_cores(slopes):
        sent = contract_last(slopes[tokens:], up).astype(BF16)
        got = swap(sent, "tp", 1)
        kept = contract_last(slopes[:tokens], up) + got.astype(F32)
        return kept.astype(BF16).reshape(2, n_fs, part, width)

    def over_places(kept):
        left, right = kept[..., :half], kept[..., half:]
        got_left = swap(left[:, 1::2], "fs", 1)
        got_right = swap(right[:, 2:], "fs", 2)
        left, right = add(left[:, ::2], got_left), add(right[:, :2], got_right)
        got_left = swap(left[:, 1], "fs", 2)
        got_right = swap(right[:, 1], "fs", 1)
        return jnp.concatenate([add(left[:, 0], got_left), add(right[:, 0], got_right)], -1)

    h_first, c_first = gather_rows(mine, theirs, ("near", "far"))
    h_last, c_last = gather_rows(mine, theirs, ("across", "own"))
    active_first = active_units(h_first)
    active_last = active_units(h_last)
    hidden_first = (active_first * active_first).astype(BF16)
    hidden_last = (active_last * active_last).astype(BF16)
    slopes_first = slopes_of(active_first, c_first)
    kept_first = between_cores(slopes_first)
    slopes_last = slopes_of(active_last, c_last)
    kept_last = between_cores(slopes_last)
    first = over_places(kept_first)
    last = over_places(kept_last)
    across_sum = add(last[0], swap(first[1], "rep", 1))
    own_sum = last[1].astype(F32) + swap(first[0], "rep", 1).astype(F32)
    final = (own_sum + swap(across_sum, "rep", 3).astype(F32)).astype(BF16)
    blocks = [final] + [swap(final, "fs", b) for b in (1, 2, 3)]
    ours = jnp.zeros((side, width), BF16)
    for b, value in enumerate(blocks):
        ours = put(ours, value, at_block[b], 0)
    others = swap(ours, "tp", 1)
    input_grad = jnp.zeros((tokens, width), BF16)
    input_grad = put(put(input_grad, ours, at_side[0], 0), others, at_side[1], 0)

    up_own = (contract_first(h_first, slopes_first) + contract_first(h_last, slopes_last)).astype(BF16)
    down_own = (contract_first(hidden_first, c_first) + contract_first(hidden_last, c_last)).astype(BF16)
    ups, downs = [], []
    for j in range(n_rep):
        u = cut(up_own, at_shard[j], shard, 0)
        d = cut(down_own, at_shard[j], shard, 1)
        if j:
            u, d = swap(u, "rep", j), swap(d, "rep", j)
        ups.append(u)
        downs.append(d)
    early = (ups[:3], downs, final)
    (ups[0], ups[1], ups[2]), downs, final = lax.optimization_barrier(early)
    ups[3], ours = lax.optimization_barrier((ups[3], ours))
    up_grad = jnp.zeros((shard, cols * n_rep), F32)
    down_grad = jnp.zeros((cols * n_rep, shard), F32)
    for j in range(n_rep):
        up_grad = put(up_grad, ups[j].astype(F32), at_cols[j], 1)
        down_grad = put(down_grad, downs[j].astype(F32), at_cols[j], 0)
    return input_grad, up_grad, down_grad


def on_device(hidden_in, cotangent, w_up, w_down):
    sizes = tuple(lax.axis_size(a) for a in ("rep", "fs", "tp"))
    gathered = 2 * hidden_in.size * sizes[0] * hidden_in.dtype.itemsize
    fits = sizes == (4, 4, 2) and gathered <= GATHER_BUDGET
    plan = gathered_tokens if fits else gathered_weights
    return plan(hidden_in, cotangent, w_up, w_down)


def solution(mesh):
    return jax.shard_map(
        on_device,
        mesh=mesh,
        in_specs=(P("rep", None), P("rep", None), P("rep", ("fs", "tp")), P(("fs", "tp"), "rep")),
        out_specs=(P("rep", None), P("rep", ("fs", "tp")), P(("fs", "tp"), "rep")),
        check_vma=False,
    )
```
